32 devices in a mesh: sp: 8 (over z, y), tp: 4 (over x, core).
Axes of the slice: x: 2, y: 2, z: 4, core: 2. Of those that a mesh axis runs over, the one named last changes fastest.
Arguments:
- stream: bfloat16 [4096, 2048], P('sp', 'tp'), may hold values from -6 to 6
- doc_ids: int32 [4096], P('sp'), may hold values from 0 to 3, never falling along the last dimension, each value on 1 to 2304 neighbouring positions
- norm_gain: float32 [2, 2048], replicated, may hold values from 0.1 to 1.9
- gate_proj: bfloat16 [2, 2048, 2048], P(None, 'sp', 'tp'), may hold values from -0.125 to 0.125
- input_gate: bfloat16 [2, 2048, 2048], P(None, 'sp', 'tp'), may hold values from -0.125 to 0.125
- value_proj: bfloat16 [2, 2048, 2048], P(None, 'sp', 'tp'), may hold values from -0.125 to 0.125
- taps: float32 [2, 3, 2048], P(None, None, 'tp'), may hold values from -3 to 3
- out_proj: bfloat16 [2, 2048, 2048], P(None, 'tp', 'sp'), may hold values from -0.125 to 0.125
Outputs:
- result: bfloat16 [4096, 2048], P('sp', 'tp')
The draws below stay inside these ranges and needn't reach their ends.
Inputs may be any that keep to these rules, and one draw needn't show every extreme that they name: `doc_ids`: document numbers never fall along the sequence; each document holds 1 to 2304 positions.
All inputs are finite; a program needn't handle non-finite values.
Results may differ from the reference program's by a relative error of at most 0.03.
Values may be sent and summed in bfloat16 or wider, within the bound.
A program may use at most 64 MiB of HBM per device.

```python
import math
import jax
import jax.numpy as jnp
import numpy as np
from jax import lax

D = 2048
CW = 2048
LAYERS = 2
TOKENS = 4096
DOCS = 4
DOC_MOST = 2304
N_TP = 4


def steps_of(rng, dims, cuts, least, high):
    def one(dim, blocks):
        draws = jax.random.uniform(jax.random.fold_in(jax.random.fold_in(rng, 6), dim), (blocks,), jnp.float32, least / len(cuts), high / len(cuts))
        return jnp.repeat(jnp.exp(draws), dims[dim] // blocks).reshape((-1,) + (1,) * (len(dims) - dim - 1))

    loudness = one(*cuts[0])
    for cut in cuts[1:]:
        loudness = loudness * one(*cut)
    return loudness


def length_profile(amount, total, bound, lean):
    loads = [(1 << 20) // math.isqrt(grade ** lean) + 1 for grade in range(2, amount + 1)]
    surplus, holding = total - bound - (amount - 1), [1] * (amount - 1)
    while surplus > 0:
        candidates = [i for i in range(amount - 1) if holding[i] < bound]
        pool, left = sum([loads[i] for i in candidates]), surplus
        for i in candidates:
            addition = min(bound - holding[i], max(1, left * loads[i] // pool), surplus)
            holding[i] = holding[i] + addition
            surplus = surplus - addition
    return np.array([bound] + holding)


def ragged_sizes(own_key, amount, total, most, slope):
    if amount == 2:
        one = jax.random.randint(own_key, (), max(1, total - most), min(most, total - 1) + 1)
        return jnp.stack([one, total - one])
    sizes = jnp.asarray(length_profile(amount, total, most, slope), jnp.int32)
    pairs = (amount - 1) // 2
    source_of, taker = sizes[1:1 + 2 * pairs:2], sizes[2:2 + 2 * pairs:2]
    room = jnp.minimum(source_of - 1, most - taker)
    moved = jax.random.randint(jax.random.fold_in(own_key, 1), (pairs,), 0, 1 << 20) % (room + 1)
    sizes = sizes.at[1:1 + 2 * pairs:2].set(source_of - moved).at[2:2 + 2 * pairs:2].set(taker + moved)
    return sizes[jax.random.permutation(jax.random.fold_in(own_key, 2), amount)]


def noise(stream_key, shape, spread, limit, split=(), kind=jnp.bfloat16):
    entries = spread * jax.random.normal(stream_key, shape, jnp.float32)
    if split:
        entries = entries * steps_of(stream_key, shape, split, -0.22, 0.18)
    return jnp.clip(entries, -limit, limit).astype(kind)


def setup_inputs(seed: int = 0) -> dict:
    key_of = jax.random.split(jax.random.key(seed), 9)
    return {
        "stream": noise(key_of[0], (TOKENS, D), 1.0, 6.0, ((0, 8), (1, 4))),
        "doc_ids": jnp.searchsorted(jnp.cumsum(ragged_sizes(key_of[1], DOCS, TOKENS, DOC_MOST, 1)), jnp.arange(TOKENS), side="right").astype(jnp.int32),
        "norm_gain": jnp.clip(1.0 + 0.18 * jax.random.normal(key_of[2], (LAYERS, D), jnp.float32), 0.1, 1.9),
        "gate_proj": noise(key_of[3], (LAYERS, D, CW), D ** -0.5, 0.125, ((1, 8), (2, 4))),
        "input_gate": noise(key_of[4], (LAYERS, D, CW), D ** -0.5, 0.125, ((1, 8), (2, 4))),
        "value_proj": noise(key_of[5], (LAYERS, D, CW), D ** -0.5, 0.125, ((1, 8), (2, 4))),
        "taps": noise(key_of[6], (LAYERS, 3, CW), 0.5, 3.0, ((2, 4),), jnp.float32),
        "out_proj": noise(key_of[7], (LAYERS, CW, D), CW ** -0.5, 0.125, ((1, 4), (2, 8))),
    }


epsilon = 1e-06

def reference(stream, doc_ids, norm_gain, gate_proj, input_gate, value_proj, taps, out_proj):
    block = CW // N_TP
    current = stream
    for layer_index in range(LAYERS):
        widened = current.astype(jnp.float32)
        scale = lax.rsqrt(lax.optimization_barrier(jnp.mean(widened * widened, axis=-1, keepdims=True)) + epsilon)
        normed = (widened * scale * norm_gain[layer_index]).astype(jnp.bfloat16)
        gate_b = jnp.dot(normed, gate_proj[layer_index], preferred_element_type=jnp.float32).astype(jnp.bfloat16)
        gate_c = jnp.dot(normed, input_gate[layer_index], preferred_element_type=jnp.float32).astype(jnp.bfloat16)
        values = jnp.dot(normed, value_proj[layer_index], preferred_element_type=jnp.float32).astype(jnp.bfloat16)
        mixed_in = (gate_c.astype(jnp.float32) * values.astype(jnp.float32)).astype(jnp.bfloat16)
        mixed_wide = mixed_in.astype(jnp.float32)
        zero_row = jnp.zeros((1, CW), jnp.float32)
        before = jnp.concatenate([zero_row, mixed_wide[:-1]], axis=0)
        after = jnp.concatenate([mixed_wide[1:], zero_row], axis=0)
        same_doc = doc_ids[1:] == doc_ids[:-1]
        false_edge = jnp.zeros((1,), bool)
        same_prev = jnp.concatenate([false_edge, same_doc])[:, None]
        same_next = jnp.concatenate([same_doc, false_edge])[:, None]
        kernel_taps = taps[layer_index]
        convolved = jnp.where(same_prev, kernel_taps[0] * before, 0.0) + kernel_taps[1] * mixed_wide + jnp.where(same_next, kernel_taps[2] * after, 0.0)
        gated = (gate_b.astype(jnp.float32) * convolved).astype(jnp.bfloat16)
        total = jnp.zeros((TOKENS, D), jnp.float32)
        for block_index in range(N_TP):
            lower = block_index * block
            partial_value = jnp.dot(gated[:, lower:lower + block], out_proj[layer_index][lower:lower + block], preferred_element_type=jnp.float32).astype(jnp.bfloat16)
            total = total + partial_value.astype(jnp.float32)
        current = (current.astype(jnp.float32) + total).astype(jnp.bfloat16)
    return current
```

```python
import functools

import jax
import jax.numpy as jnp
from jax import lax
from jax.experimental import pallas as pl
from jax.experimental.pallas import tpu as pltpu
from jax.sharding import PartitionSpec as P

epsilon = 1e-06


def with_halo(value, sides, width):
    for axis, dim in sides:
        size, length = (lax.axis_size(axis), value.shape[dim])
        up = [(i, (i + 1) % size) for i in range(size - 1)]
        down = [(j, i) for i, j in up]
        last = lax.slice_in_dim(value, length - width, length, axis=dim)
        leading = lax.slice_in_dim(value, 0, width, axis=dim)
        before = lax.ppermute(last, axis, up)
        after = lax.ppermute(leading, axis, down)
        value = jnp.concatenate([before, value, after], axis=dim)
    return value


def per_device(stream, doc_ids, norm_gain, gate_proj, input_gate, value_proj, taps, out_proj):
    layers = gate_proj.shape[0]
    gathered_in = (
        lax.all_gather(gate_proj, "sp", axis=1, tiled=True),
        lax.all_gather(input_gate, "sp", axis=1, tiled=True),
        lax.all_gather(value_proj, "sp", axis=1, tiled=True),
    )
    gathered_out = lax.all_gather(out_proj, "sp", axis=2, tiled=True)
    current = stream
    for layer_index in range(layers):
        full_rows = lax.all_gather(current, "tp", axis=1, tiled=True)
        widened = full_rows.astype(jnp.float32)
        scale = lax.rsqrt(jnp.mean(widened * widened, axis=-1, keepdims=True) + epsilon)
        normed = (widened * scale * norm_gain[layer_index]).astype(jnp.bfloat16)
        gate_b = jnp.dot(normed, gathered_in[0][layer_index], preferred_element_type=jnp.float32)
        gate_c = jnp.dot(normed, gathered_in[1][layer_index], preferred_element_type=jnp.float32)
        values = jnp.dot(normed, gathered_in[2][layer_index], preferred_element_type=jnp.float32)
        gate_b = gate_b.astype(jnp.bfloat16)
        gate_c = gate_c.astype(jnp.bfloat16)
        values = values.astype(jnp.bfloat16)
        mixed_in = (gate_c.astype(jnp.float32) * values.astype(jnp.float32)).astype(jnp.bfloat16)
        padded, doc_padded = (
            with_halo(mixed_in, (("sp", 0),), 1),
            with_halo(doc_ids, (("sp", 0),), 1),
        )
        same_prev = (doc_padded[:-2] == doc_ids)[:, None]
        same_next = (doc_padded[2:] == doc_ids)[:, None]
        kernel_taps = taps[layer_index]
        convolved = (
            jnp.where(same_prev, kernel_taps[0] * padded[:-2].astype(jnp.float32), 0.0)
            + kernel_taps[1] * mixed_in.astype(jnp.float32)
            + jnp.where(same_next, kernel_taps[2] * padded[2:].astype(jnp.float32), 0.0)
        )
        gated = (gate_b.astype(jnp.float32) * convolved).astype(jnp.bfloat16)
        partials = jnp.dot(gated, gathered_out[layer_index], preferred_element_type=jnp.float32)
        summed = lax.psum_scatter(
            partials.astype(jnp.bfloat16), "tp", scatter_dimension=1, tiled=True
        ).astype(jnp.float32)
        current = (current.astype(jnp.float32) + summed).astype(jnp.bfloat16)
    return current


MESH = pl.DeviceIdType.MESH


def fused_kernel(S, T, L, stream_ref, docs_ref, gain_ref, gate_ref, input_ref, value_ref, taps_ref, outw_ref,
                 result_ref, win, wout, xfull, normed, cbuf, mpad, edge, halo, docpad, dhalo, mprev, mnext,
                 gated, pbuf, rbuf, own_sem, w_send, w_recv, ag_send, ag_recv, rs_send, rs_recv,
                 h_send, h_recv, d_send, d_recv, x_sem):
    s = lax.axis_index("sp")
    t = lax.axis_index("tp")
    Z = S // 2
    z, y = s // 2, s % 2
    rows, width = stream_ref.shape
    depth = gate_ref.shape[1]
    cols = taps_ref.shape[2]
    ow = outw_ref.shape[2]
    per = S // T
    units = 4 * L
    mate = z + 1 - 2 * (z % 2)
    sources = (input_ref, value_ref, gate_ref)
    sends = []

    barrier = pltpu.get_barrier_semaphore()

    def greet(sp_index, tp_index):
        pl.semaphore_signal(barrier, inc=1, device_id=(sp_index, tp_index), device_id_type=MESH)

    nxt, prv = lax.rem(s + 1, S), lax.rem(s + S - 1, S)
    greet(2 * z + 1 - y, t)
    greet(nxt, t)
    greet(prv, t)
    for k in range(1, T):
        greet(s, lax.rem(t + k, T))

    @pl.when(z > 0)
    def _():
        greet(s - 2, t)

    @pl.when(z < Z - 1)
    def _():
        greet(s + 2, t)

    def slot(u, shard):
        layer, part = u // 4, u % 4
        if part < 3:
            return win.at[layer * 3 + part, pl.ds(pl.multiple_of(shard * depth, depth), depth)]
        return wout.at[layer, shard]

    def own_copy(u):
        layer, part = u // 4, u % 4
        source = outw_ref.at[layer] if part == 3 else sources[part].at[layer]
        return pltpu.make_async_copy(source, slot(u, s), own_sem.at[u])

    x_copy = pltpu.make_async_copy(stream_ref, xfull.at[0, t], x_sem)
    x_copy.start()
    for u in range(units):
        own_copy(u).start()

    pl.semaphore_wait(barrier, T + 2 + jnp.where(z > 0, 1, 0) + jnp.where(z < Z - 1, 1, 0))

    def w_copy(u, shard, way):
        target = (s + 2, s - 2, 2 * z + 1 - y)[way]
        return pltpu.make_async_remote_copy(
            src_ref=slot(u, shard), dst_ref=slot(u, shard),
            send_sem=w_send.at[way, u, shard], recv_sem=w_recv.at[u, shard],
            device_id=(target, t), device_id_type=MESH)

    def send(cond, copy_of):
        @pl.when(cond)
        def _():
            copy_of().start()
        sends.append((cond, copy_of))

    def arrived(u, shard):
        w_copy(u, shard, 2).wait_recv()

    def own(u):
        own_copy(u).wait()
        send(z < Z - 1, lambda: w_copy(u, s, 0))
        send(z > 0, lambda: w_copy(u, s, 1))
        send(z >= 0, lambda: w_copy(u, s, 2))

    def forward(u):
        if u >= units:
            return
        if u + 2 < units:
            own(u + 2)
        through_mate = u % 2 == 1 and Z % 2 == 0
        other = 2 * z + 1 - y
        if through_mate:
            arrived(u, other)
            send(z % 2 == 0, lambda: w_copy(u, other, 0))
            send(z % 2 == 1, lambda: w_copy(u, other, 1))
        for d in range(1, Z):
            for sign in (-1, 1):
                at = z + sign * d
                exists = (at >= 0) if sign < 0 else (at < Z)
                shard = 2 * at + y

                @pl.when(exists)
                def _():
                    arrived(u, shard)

                onward = (z < Z - 1) if sign < 0 else (z > 0)
                send(jnp.logical_and(exists, onward), lambda shard=shard, sign=sign: w_copy(u, shard, 0 if sign < 0 else 1))
                across = jnp.logical_and(exists, at != mate) if through_mate and d == 1 else exists
                send(across, lambda shard=shard: w_copy(u, shard, 2))

    def others(u, use):
        through_mate = u % 2 == 1 and Z % 2 == 0

        def step(e, carry):
            at = z + (1 - 2 * (e % 2)) * ((e + 1) // 2)
            shard = 2 * at + 1 - y
            inside = jnp.logical_and(at >= 0, at < Z)
            fresh = jnp.logical_and(inside, e > 0) if through_mate else inside

            @pl.when(fresh)
            def _():
                arrived(u, shard)

            if use is not None:
                @pl.when(inside)
                def _():
                    use(shard)
            return carry

        lax.fori_loop(0, 2 * Z - 1, step, 0)

    def ag_copy(layer, k):
        return pltpu.make_async_remote_copy(
            src_ref=xfull.at[layer, t], dst_ref=xfull.at[layer, t],
            send_sem=ag_send.at[layer, k], recv_sem=ag_recv.at[layer, t],
            device_id=(s, lax.rem(t + k, T)), device_id_type=MESH)

    def ag_wait(layer):
        for k in range(1, T):
            q = lax.rem(t + k, T)
            pltpu.make_async_remote_copy(
                src_ref=xfull.at[layer, q], dst_ref=xfull.at[layer, q],
                send_sem=ag_send.at[layer, k], recv_sem=ag_recv.at[layer, q],
                device_id=(s, q), device_id_type=MESH).wait_recv()

    def ag_start(layer):
        for k in range(1, T):
            ag_copy(layer, k).start()

    def halo_copy(layer, side):
        return pltpu.make_async_remote_copy(
            src_ref=edge.at[layer, 1 - side], dst_ref=halo.at[layer, side],
            send_sem=h_send.at[layer, side], recv_sem=h_recv.at[layer, side],
            device_id=((nxt, prv)[side], t), device_id_type=MESH)

    def doc_copy(side):
        return pltpu.make_async_remote_copy(
            src_ref=docs_ref.at[pl.ds((rows - 8, 0)[side], 8)], dst_ref=dhalo.at[side],
            send_sem=d_send.at[side], recv_sem=d_recv.at[side],
            device_id=((nxt, prv)[side], t), device_id_type=MESH)

    x_copy.wait()
    own(0)
    ag_start(0)
    own(1)
    for side in range(2):
        doc_copy(side).start()

    tile = rows // 2
    small = rows // 8

    def norm(layer):
        def step(r, carry):
            at = pl.ds(pl.multiple_of(r * small, small), small)
            total = jnp.zeros((small, 1), jnp.float32)
            for q in range(T):
                wide = xfull[layer, q, at, :].astype(jnp.float32)
                total = total + jnp.sum(wide * wide, axis=-1, keepdims=True)
            scale = lax.rsqrt(total / (width * T) + epsilon)
            for q in range(T):
                wide = xfull[layer, q, at, :].astype(jnp.float32)
                gain = gain_ref[layer:layer + 1, q * width:(q + 1) * width]
                normed[at, q * width:(q + 1) * width] = (wide * scale * gain).astype(jnp.bfloat16)
            return carry

        lax.fori_loop(0, rows // small, step, 0)

    def project(layer, part, use):
        def step(r, carry):
            start = pl.multiple_of(r * tile, tile)
            at = pl.ds(start, tile)
            product = jnp.dot(normed[at, :], win[layer * 3 + part], preferred_element_type=jnp.float32)
            use(at, start, product.astype(jnp.bfloat16))
            return carry

        lax.fori_loop(0, rows // tile, step, 0)

    def keep_gate(at, start, value):
        cbuf[at, :] = value

    def mix(at, start, value):
        mixed = (cbuf[at, :].astype(jnp.float32) * value.astype(jnp.float32)).astype(jnp.bfloat16)
        mpad[pl.ds(start + 8, tile), :] = mixed.astype(jnp.float32)

    def masks():
        for side in range(2):
            doc_copy(side).wait_recv()
        docpad[8:8 + rows, :] = docs_ref[...]
        docpad[7:8, :] = jnp.where(s > 0, dhalo[0, 7:8, :], -1)
        docpad[8 + rows:9 + rows, :] = jnp.where(s < S - 1, dhalo[1, 0:1, :], -1)
        mprev[...] = jnp.where(docpad[7:7 + rows, :] == docs_ref[...], 1.0, 0.0)
        mnext[...] = jnp.where(docpad[9:9 + rows, :] == docs_ref[...], 1.0, 0.0)

    def convolve(layer):
        for side in range(2):
            halo_copy(layer, side).wait_recv()
        mpad[7:8, :] = halo[layer, 0, 15:16, :].astype(jnp.float32)
        mpad[8 + rows:9 + rows, :] = halo[layer, 1, 0:1, :].astype(jnp.float32)
        for low in range(0, cols, 128):
            lanes = slice(low, low + 128)
            for r in range(0, rows, small):
                before = taps_ref[layer, 0:1, lanes] * mpad[r + 7:r + 7 + small, lanes]
                middle = taps_ref[layer, 1:2, lanes] * mpad[r + 8:r + 8 + small, lanes]
                after = taps_ref[layer, 2:3, lanes] * mpad[r + 9:r + 9 + small, lanes]
                here = slice(r, r + small)
                total = (jnp.where(mprev[here, :] > 0.5, before, 0.0) + middle
                         + jnp.where(mnext[here, :] > 0.5, after, 0.0))
                gated[here, lanes] = (cbuf[here, lanes].astype(jnp.float32) * total).astype(jnp.bfloat16)

    def rs_copy(layer, shard):
        return pltpu.make_async_remote_copy(
            src_ref=pbuf.at[layer, shard], dst_ref=rbuf.at[layer, t, shard % per],
            send_sem=rs_send.at[layer, shard], recv_sem=rs_recv.at[layer, t, shard % per],
            device_id=(s, shard // per), device_id_type=MESH)

    def out_block(layer, shard):
        part = jnp.dot(gated[...], wout[layer, shard], preferred_element_type=jnp.float32)
        pbuf[layer, shard] = part.astype(jnp.bfloat16)

        @pl.when(shard // per != t)
        def _():
            rs_copy(layer, shard).start()

    def finish(layer):
        for i in range(per):
            for k in range(1, T):
                q = lax.rem(t + k, T)
                pltpu.make_async_remote_copy(
                    src_ref=rbuf.at[layer, q, i], dst_ref=rbuf.at[layer, q, i],
                    send_sem=rs_send.at[layer, i], recv_sem=rs_recv.at[layer, q, i],
                    device_id=(s, q), device_id_type=MESH).wait_recv()

        def step(r, carry):
            at = pl.ds(pl.multiple_of(r * small, small), small)
            for i in range(per):
                lanes = slice(i * ow, (i + 1) * ow)
                total = pbuf[layer, t * per + i, at, :].astype(jnp.float32)
                for k in range(1, T):
                    total = total + rbuf[layer, lax.rem(t + k, T), i, at, :].astype(jnp.float32)
                fresh = (xfull[layer, t, at, lanes].astype(jnp.float32) + total).astype(jnp.bfloat16)
                if layer + 1 < L:
                    xfull[layer + 1, t, at, lanes] = fresh
                else:
                    result_ref[at, lanes] = fresh
            return carry

        lax.fori_loop(0, rows // small, step, 0)

    forward(0)
    forward(1)
    for layer in range(L):
        base = 4 * layer
        forward(base + 2)
        ag_wait(layer)
        norm(layer)
        others(base, None)
        project(layer, 0, keep_gate)
        others(base + 1, None)
        project(layer, 1, mix)
        edge[layer, 0] = mpad[8:24, :].astype(jnp.bfloat16)
        edge[layer, 1] = mpad[rows - 8:rows + 8, :].astype(jnp.bfloat16)
        for side in range(2):
            halo_copy(layer, side).start()
        if layer == 0:
            masks()
        forward(base + 3)
        others(base + 2, None)
        project(layer, 2, keep_gate)
        convolve(layer)
        forward(base + 4)

        def column(at, carry):
            out_block(layer, 2 * at + y)
            return carry

        lax.fori_loop(0, Z, column, 0)
        others(base + 3, functools.partial(out_block, layer))
        forward(base + 5)
        finish(layer)
        if layer + 1 < L:
            ag_start(layer + 1)

    for cond, copy_of in sends:
        @pl.when(cond)
        def _():
            copy_of().wait_send()
    for layer in range(L):
        for k in range(1, T):
            ag_copy(layer, k).wait_send()
        for side in range(2):
            halo_copy(layer, side).wait_send()

        def drain(shard, carry):
            @pl.when(shard // per != t)
            def _():
                rs_copy(layer, shard).wait_send()
            return carry

        lax.fori_loop(0, S, drain, 0)
    for side in range(2):
        doc_copy(side).wait_send()


def fused(S, T, stream, doc_ids, norm_gain, gate_proj, input_gate, value_proj, taps, out_proj):
    rows, width = stream.shape
    L, depth, cols = gate_proj.shape
    ow = out_proj.shape[2]
    bf, f32, i32 = jnp.bfloat16, jnp.float32, jnp.int32
    docs = jnp.broadcast_to(doc_ids[:, None], (rows, 128))
    vmem, hbm = pl.BlockSpec(memory_space=pltpu.VMEM), pl.BlockSpec(memory_space=pl.ANY)
    dma = pltpu.SemaphoreType.DMA
    scratch = [
        pltpu.VMEM((3 * L, S * depth, cols), bf),
        pltpu.VMEM((L, S, cols, ow), bf),
        pltpu.VMEM((L, T, rows, width), bf),
        pltpu.VMEM((rows, T * width), bf),
        pltpu.VMEM((rows, cols), bf),
        pltpu.VMEM((rows + 16, cols), f32),
        pltpu.VMEM((L, 2, 16, cols), bf),
        pltpu.VMEM((L, 2, 16, cols), bf),
        pltpu.VMEM((rows + 16, 128), i32),
        pltpu.VMEM((2, 8, 128), i32),
        pltpu.VMEM((rows, 128), f32),
        pltpu.VMEM((rows, 128), f32),
        pltpu.VMEM((rows, cols), bf),
        pltpu.VMEM((L, S, rows, ow), bf),
        pltpu.VMEM((L, T, S // T, rows, ow), bf),
        dma((4 * L,)),
        dma((3, 4 * L, S)),
        dma((4 * L, S)),
        dma((L, T)),
        dma((L, T)),
        dma((L, S)),
        dma((L, T, S // T)),
        dma((L, 2)),
        dma((L, 2)),
        dma((2,)),
        dma((2,)),
        dma,
    ]
    return pl.pallas_call(
        functools.partial(fused_kernel, S, T, L),
        out_shape=jax.ShapeDtypeStruct((rows, width), bf),
        in_specs=[hbm, vmem, vmem, hbm, hbm, hbm, vmem, hbm],
        out_specs=vmem,
        scratch_shapes=scratch,
        compiler_params=pltpu.CompilerParams(
            collective_id=0, has_side_effects=True, vmem_limit_bytes=60 * 1024 * 1024),
    )(stream, docs, norm_gain, gate_proj, input_gate, value_proj, taps, out_proj)


def solution(mesh):
    sp, tp = mesh.shape["sp"], mesh.shape["tp"]

    def body(*arrays):
        out_width = arrays[7].shape[2]
        if out_width % 128 == 0 and sp % 2 == 0 and sp % tp == 0:
            return fused(sp, tp, *arrays)
        return per_device(*arrays)

    in_specs = (
        P("sp", "tp"),
        P("sp"),
        P(),
        P(None, "sp", "tp"),
        P(None, "sp", "tp"),
        P(None, "sp", "tp"),
        P(None, None, "tp"),
        P(None, "tp", "sp"),
    )
    out_specs = P("sp", "tp")
    return jax.shard_map(
        body, mesh=mesh, in_specs=in_specs, out_specs=out_specs, check_vma=False
    )
```

```python
import functools

import jax
import jax.numpy as jnp
from jax import lax
from jax.experimental import pallas as pl
from jax.experimental.pallas import tpu as pltpu
from jax.sharding import PartitionSpec as P

epsilon = 1e-06


def with_halo(value, sides, width):
    for axis, dim in sides:
        size, length = (lax.axis_size(axis), value.shape[dim])
        up = [(i, (i + 1) % size) for i in range(size - 1)]
        down = [(j, i) for i, j in up]
        last = lax.slice_in_dim(value, length - width, length, axis=dim)
        leading = lax.slice_in_dim(value, 0, width, axis=dim)
        before = lax.ppermute(last, axis, up)
        after = lax.ppermute(leading, axis, down)
        value = jnp.concatenate([before, value, after], axis=dim)
    return value


def per_device(stream, doc_ids, norm_gain, gate_proj, input_gate, value_proj, taps, out_proj):
    layers = gate_proj.shape[0]
    gathered_in = (
        lax.all_gather(gate_proj, "sp", axis=1, tiled=True),
        lax.all_gather(input_gate, "sp", axis=1, tiled=True),
        lax.all_gather(value_proj, "sp", axis=1, tiled=True),
    )
    gathered_out = lax.all_gather(out_proj, "sp", axis=2, tiled=True)
    current = stream
    for layer_index in range(layers):
        full_rows = lax.all_gather(current, "tp", axis=1, tiled=True)
        widened = full_rows.astype(jnp.float32)
        scale = lax.rsqrt(jnp.mean(widened * widened, axis=-1, keepdims=True) + epsilon)
        normed = (widened * scale * norm_gain[layer_index]).astype(jnp.bfloat16)
        gate_b = jnp.dot(normed, gathered_in[0][layer_index], preferred_element_type=jnp.float32)
        gate_c = jnp.dot(normed, gathered_in[1][layer_index], preferred_element_type=jnp.float32)
        values = jnp.dot(normed, gathered_in[2][layer_index], preferred_element_type=jnp.float32)
        gate_b = gate_b.astype(jnp.bfloat16)
        gate_c = gate_c.astype(jnp.bfloat16)
        values = values.astype(jnp.bfloat16)
        mixed_in = (gate_c.astype(jnp.float32) * values.astype(jnp.float32)).astype(jnp.bfloat16)
        padded, doc_padded = (
            with_halo(mixed_in, (("sp", 0),), 1),
            with_halo(doc_ids, (("sp", 0),), 1),
        )
        same_prev = (doc_padded[:-2] == doc_ids)[:, None]
        same_next = (doc_padded[2:] == doc_ids)[:, None]
        kernel_taps = taps[layer_index]
        convolved = (
            jnp.where(same_prev, kernel_taps[0] * padded[:-2].astype(jnp.float32), 0.0)
            + kernel_taps[1] * mixed_in.astype(jnp.float32)
            + jnp.where(same_next, kernel_taps[2] * padded[2:].astype(jnp.float32), 0.0)
        )
        gated = (gate_b.astype(jnp.float32) * convolved).astype(jnp.bfloat16)
        partials = jnp.dot(gated, gathered_out[layer_index], preferred_element_type=jnp.float32)
        summed = lax.psum_scatter(
            partials.astype(jnp.bfloat16), "tp", scatter_dimension=1, tiled=True
        ).astype(jnp.float32)
        current = (current.astype(jnp.float32) + summed).astype(jnp.bfloat16)
    return current


MESH = pl.DeviceIdType.MESH


def fused_kernel(S, T, L, stream_ref, docs_ref, gain_ref, gate_ref, input_ref, value_ref, taps_ref, outw_ref,
                 result_ref, win, wout, xfull, normed, cbuf, mpad, edge, halo, docpad, dhalo, mprev, mnext,
                 gated, pbuf, rbuf, own_sem, w_send, w_recv, ag_send, ag_recv, rs_send, rs_recv, sbuf, p_send, p_recv,
                 h_send, h_recv, d_send, d_recv, x_sem):
    s = lax.axis_index("sp")
    t = lax.axis_index("tp")
    Z = S // 2
    z, y = s // 2, s % 2
    rows, width = stream_ref.shape
    depth = gate_ref.shape[1]
    cols = taps_ref.shape[2]
    ow = outw_ref.shape[2]
    per = S // T
    units = 4 * L
    sibling = t + 1 - 2 * (t % 2)
    adders = [sibling] + [lax.rem(t + k, T) for k in range(2, T, 2)]
    mate = z + 1 - 2 * (z % 2)
    sources = (input_ref, value_ref, gate_ref)
    sends = []

    barrier = pltpu.get_barrier_semaphore()

    def greet(sp_index, tp_index):
        pl.semaphore_signal(barrier, inc=1, device_id=(sp_index, tp_index), device_id_type=MESH)

    nxt, prv = lax.rem(s + 1, S), lax.rem(s + S - 1, S)
    greet(2 * z + 1 - y, t)
    greet(nxt, t)
    greet(prv, t)
    for k in range(1, T):
        greet(s, lax.rem(t + k, T))

    @pl.when(z > 0)
    def _():
        greet(s - 2, t)

    @pl.when(z < Z - 1)
    def _():
        greet(s + 2, t)

    def slot(u, shard):
        layer, part = u // 4, u % 4
        if part < 3:
            return win.at[layer * 3 + part, pl.ds(pl.multiple_of(shard * depth, depth), depth)]
        return wout.at[layer, shard]

    def own_copy(u):
        layer, part = u // 4, u % 4
        source = outw_ref.at[layer] if part == 3 else sources[part].at[layer]
        return pltpu.make_async_copy(source, slot(u, s), own_sem.at[u])

    x_copy = pltpu.make_async_copy(stream_ref, xfull.at[0, t], x_sem)
    x_copy.start()
    for u in range(units):
        own_copy(u).start()

    pl.semaphore_wait(barrier, T + 2 + jnp.where(z > 0, 1, 0) + jnp.where(z < Z - 1, 1, 0))

    def w_copy(u, shard, way):
        target = (s + 2, s - 2, 2 * z + 1 - y)[way]
        return pltpu.make_async_remote_copy(
            src_ref=slot(u, shard), dst_ref=slot(u, shard),
            send_sem=w_send.at[way, u, shard], recv_sem=w_recv.at[u, shard],
            device_id=(target, t), device_id_type=MESH)

    def send(cond, copy_of):
        @pl.when(cond)
        def _():
            copy_of().start()
        sends.append((cond, copy_of))

    def arrived(u, shard):
        w_copy(u, shard, 2).wait_recv()

    def own(u):
        own_copy(u).wait()
        send(z < Z - 1, lambda: w_copy(u, s, 0))
        send(z > 0, lambda: w_copy(u, s, 1))
        send(z >= 0, lambda: w_copy(u, s, 2))

    def forward(u, whole=True):
        if u >= units:
            return
        if u + 1 < units:
            own(u + 1)
        through_mate = u % 2 == 1 and Z % 2 == 0
        other = 2 * z + 1 - y
        if through_mate:
            arrived(u, other)
            send(z % 2 == 0, lambda: w_copy(u, other, 0))
            send(z % 2 == 1, lambda: w_copy(u, other, 1))
        for d in range(1, Z if whole else 2):
            onward_step(u, d)

    def onward_step(u, d):
        through_mate = u % 2 == 1 and Z % 2 == 0
        for sign in (-1, 1):
            at = z + sign * d
            exists = (at >= 0) if sign < 0 else (at < Z)
            shard = 2 * at + y

            @pl.when(exists)
            def _():
                arrived(u, shard)

            onward = (z < Z - 1) if sign < 0 else (z > 0)
            send(jnp.logical_and(exists, onward), lambda shard=shard, sign=sign: w_copy(u, shard, 0 if sign < 0 else 1))
            across = jnp.logical_and(exists, at != mate) if through_mate and d == 1 else exists
            send(across, lambda shard=shard: w_copy(u, shard, 2))

    def others(u, use):
        through_mate = u % 2 == 1 and Z % 2 == 0

        def step(e, carry):
            at = z + (1 - 2 * (e % 2)) * ((e + 1) // 2)
            shard = 2 * at + 1 - y
            inside = jnp.logical_and(at >= 0, at < Z)
            fresh = jnp.logical_and(inside, e > 0) if through_mate else inside

            @pl.when(fresh)
            def _():
                arrived(u, shard)

            if use is not None:
                @pl.when(inside)
                def _():
                    use(shard)
            return carry

        lax.fori_loop(0, 2 * Z - 1, step, 0)

    def ag_copy(layer, k):
        return pltpu.make_async_remote_copy(
            src_ref=xfull.at[layer, t], dst_ref=xfull.at[layer, t],
            send_sem=ag_send.at[layer, k], recv_sem=ag_recv.at[layer, t],
            device_id=(s, lax.rem(t + k, T)), device_id_type=MESH)

    def ag_wait(layer):
        for k in range(1, T):
            q = lax.rem(t + k, T)
            pltpu.make_async_remote_copy(
                src_ref=xfull.at[layer, q], dst_ref=xfull.at[layer, q],
                send_sem=ag_send.at[layer, k], recv_sem=ag_recv.at[layer, q],
                device_id=(s, q), device_id_type=MESH).wait_recv()

    def ag_start(layer):
        for k in range(1, T):
            ag_copy(layer, k).start()

    def halo_copy(layer, side):
        return pltpu.make_async_remote_copy(
            src_ref=edge.at[layer, 1 - side], dst_ref=halo.at[layer, side],
            send_sem=h_send.at[layer, side], recv_sem=h_recv.at[layer, side],
            device_id=((nxt, prv)[side], t), device_id_type=MESH)

    def doc_copy(side):
        return pltpu.make_async_remote_copy(
            src_ref=docs_ref.at[pl.ds((rows - 8, 0)[side], 8)], dst_ref=dhalo.at[side],
            send_sem=d_send.at[side], recv_sem=d_recv.at[side],
            device_id=((nxt, prv)[side], t), device_id_type=MESH)

    x_copy.wait()
    own(0)
    ag_start(0)
    for side in range(2):
        doc_copy(side).start()

    tile = rows // 2
    small = rows // 8

    def norm(layer):
        def step(r, carry):
            at = pl.ds(pl.multiple_of(r * small, small), small)
            total = jnp.zeros((small, 1), jnp.float32)
            for q in range(T):
                wide = xfull[layer, q, at, :].astype(jnp.float32)
                total = total + jnp.sum(wide * wide, axis=-1, keepdims=True)
            scale = lax.rsqrt(total / (width * T) + epsilon)
            for q in range(T):
                wide = xfull[layer, q, at, :].astype(jnp.float32)
                gain = gain_ref[layer:layer + 1, q * width:(q + 1) * width]
                normed[at, q * width:(q + 1) * width] = (wide * scale * gain).astype(jnp.bfloat16)
            return carry

        lax.fori_loop(0, rows // small, step, 0)

    def project(layer, part, use):
        def step(r, carry):
            start = pl.multiple_of(r * tile, tile)
            at = pl.ds(start, tile)
            product = jnp.dot(normed[at, :], win[layer * 3 + part], preferred_element_type=jnp.float32)
            use(at, start, product.astype(jnp.bfloat16))
            return carry

        lax.fori_loop(0, rows // tile, step, 0)

    def keep_gate(at, start, value):
        cbuf[at, :] = value

    def mix(at, start, value):
        mixed = (cbuf[at, :].astype(jnp.float32) * value.astype(jnp.float32)).astype(jnp.bfloat16)
        mpad[pl.ds(start + 8, tile), :] = mixed.astype(jnp.float32)

    def masks():
        for side in range(2):
            doc_copy(side).wait_recv()
        docpad[8:8 + rows, :] = docs_ref[...]
        docpad[7:8, :] = jnp.where(s > 0, dhalo[0, 7:8, :], -1)
        docpad[8 + rows:9 + rows, :] = jnp.where(s < S - 1, dhalo[1, 0:1, :], -1)
        mprev[...] = jnp.where(docpad[7:7 + rows, :] == docs_ref[...], 1.0, 0.0)
        mnext[...] = jnp.where(docpad[9:9 + rows, :] == docs_ref[...], 1.0, 0.0)

    def convolve(layer):
        for side in range(2):
            halo_copy(layer, side).wait_recv()
        mpad[7:8, :] = halo[layer, 0, 15:16, :].astype(jnp.float32)
        mpad[8 + rows:9 + rows, :] = halo[layer, 1, 0:1, :].astype(jnp.float32)
        for low in range(0, cols, 128):
            lanes = slice(low, low + 128)
            for r in range(0, rows, small):
                before = taps_ref[0, layer:layer + 1, lanes] * mpad[r + 7:r + 7 + small, lanes]
                middle = taps_ref[1, layer:layer + 1, lanes] * mpad[r + 8:r + 8 + small, lanes]
                after = taps_ref[2, layer:layer + 1, lanes] * mpad[r + 9:r + 9 + small, lanes]
                here = slice(r, r + small)
                total = (jnp.where(mprev[here, :] > 0.5, before, 0.0) + middle
                         + jnp.where(mnext[here, :] > 0.5, after, 0.0))
                gated[here, lanes] = (cbuf[here, lanes].astype(jnp.float32) * total).astype(jnp.bfloat16)

    def rs_copy(layer, shard):
        return pltpu.make_async_remote_copy(
            src_ref=pbuf.at[layer, shard], dst_ref=rbuf.at[layer, t, shard % per],
            send_sem=rs_send.at[layer, shard], recv_sem=rs_recv.at[layer, t, shard % per],
            device_id=(s, shard // per), device_id_type=MESH)

    def pair_copy(layer, shard):
        return pltpu.make_async_remote_copy(
            src_ref=pbuf.at[layer, shard], dst_ref=sbuf.at[layer, shard],
            send_sem=p_send.at[layer, shard], recv_sem=p_recv.at[layer, shard],
            device_id=(s, sibling), device_id_type=MESH)

    def out_block(layer, shard):
        part = jnp.dot(gated[...], wout[layer, shard], preferred_element_type=jnp.float32)
        pbuf[layer, shard] = part.astype(jnp.bfloat16)

        owner = shard // per
        near, same = owner // 2 == t // 2, owner % 2 == t % 2

        @pl.when(jnp.logical_and(jnp.logical_not(near), jnp.logical_not(same)))
        def _():
            pair_copy(layer, shard).start()

        @pl.when(jnp.logical_and(jnp.logical_not(near), same))
        def _():
            pair_copy(layer, shard).wait_recv()
            both = part + sbuf[layer, shard].astype(jnp.float32)
            pbuf[layer, shard] = both.astype(jnp.bfloat16)

        @pl.when(near != same)
        def _():
            rs_copy(layer, shard).start()

    def finish(layer):
        for i in range(per):
            for q in adders:
                pltpu.make_async_remote_copy(
                    src_ref=rbuf.at[layer, q, i], dst_ref=rbuf.at[layer, q, i],
                    send_sem=rs_send.at[layer, i], recv_sem=rs_recv.at[layer, q, i],
                    device_id=(s, q), device_id_type=MESH).wait_recv()

        def step(r, carry):
            at = pl.ds(pl.multiple_of(r * small, small), small)
            for i in range(per):
                lanes = slice(i * ow, (i + 1) * ow)
                total = pbuf[layer, t * per + i, at, :].astype(jnp.float32)
                for q in adders:
                    total = total + rbuf[layer, q, i, at, :].astype(jnp.float32)
                fresh = (xfull[layer, t, at, lanes].astype(jnp.float32) + total).astype(jnp.bfloat16)
                if layer + 1 < L:
                    xfull[layer + 1, t, at, lanes] = fresh
                else:
                    result_ref[at, lanes] = fresh
            return carry

        lax.fori_loop(0, rows // small, step, 0)

    forward(0)
    forward(1)
    for layer in range(L):
        base = 4 * layer
        forward(base + 2)
        ag_wait(layer)
        norm(layer)
        others(base, None)
        project(layer, 0, keep_gate)
        others(base + 1, None)
        project(layer, 1, mix)
        edge[layer, 0] = mpad[8:24, :].astype(jnp.bfloat16)
        edge[layer, 1] = mpad[rows - 8:rows + 8, :].astype(jnp.bfloat16)
        for side in range(2):
            halo_copy(layer, side).start()
        if layer == 0:
            masks()
        last = layer == L - 1
        forward(base + 3, whole=not last)
        others(base + 2, None)
        project(layer, 2, keep_gate)
        convolve(layer)
        forward(base + 4)

        def column(e, carry):
            at = z + (1 - 2 * (e % 2)) * ((e + 1) // 2)

            @pl.when(jnp.logical_and(at >= 0, at < Z))
            def _():
                out_block(layer, 2 * at + y)
            return carry

        if last:
            lax.fori_loop(0, min(3, 2 * Z - 1), column, 0)
            for d in range(2, Z):
                onward_step(base + 3, d)
                lax.fori_loop(2 * d - 1, 2 * d + 1, column, 0)
        else:
            lax.fori_loop(0, 2 * Z - 1, column, 0)
        others(base + 3, functools.partial(out_block, layer))
        forward(base + 5)
        finish(layer)
        if layer + 1 < L:
            ag_start(layer + 1)

    for cond, copy_of in sends:
        @pl.when(cond)
        def _():
            copy_of().wait_send()
    for layer in range(L):
        for k in range(1, T):
            ag_copy(layer, k).wait_send()
        for side in range(2):
            halo_copy(layer, side).wait_send()

        def drain(shard, carry):
            owner = shard // per
            near, same = owner // 2 == t // 2, owner % 2 == t % 2

            @pl.when(near != same)
            def _():
                rs_copy(layer, shard).wait_send()

            @pl.when(jnp.logical_and(jnp.logical_not(near), jnp.logical_not(same)))
            def _():
                pair_copy(layer, shard).wait_send()
            return carry

        lax.fori_loop(0, S, drain, 0)
    for side in range(2):
        doc_copy(side).wait_send()


def fused(S, T, stream, doc_ids, norm_gain, gate_proj, input_gate, value_proj, taps, out_proj):
    rows, width = stream.shape
    L, depth, cols = gate_proj.shape
    ow = out_proj.shape[2]
    bf, f32, i32 = jnp.bfloat16, jnp.float32, jnp.int32
    docs = jnp.broadcast_to(doc_ids[:, None], (rows, 128))
    vmem, hbm = pl.BlockSpec(memory_space=pltpu.VMEM), pl.BlockSpec(memory_space=pl.ANY)
    dma = pltpu.SemaphoreType.DMA
    scratch = [
        pltpu.VMEM((3 * L, S * depth, cols), bf),
        pltpu.VMEM((L, S, cols, ow), bf),
        pltpu.VMEM((L, T, rows, width), bf),
        pltpu.VMEM((rows, T * width), bf),
        pltpu.VMEM((rows, cols), bf),
        pltpu.VMEM((rows + 16, cols), f32),
        pltpu.VMEM((L, 2, 16, cols), bf),
        pltpu.VMEM((L, 2, 16, cols), bf),
        pltpu.VMEM((rows + 16, 128), i32),
        pltpu.VMEM((2, 8, 128), i32),
        pltpu.VMEM((rows, 128), f32),
        pltpu.VMEM((rows, 128), f32),
        pltpu.VMEM((rows, cols), bf),
        pltpu.VMEM((L, S, rows, ow), bf),
        pltpu.VMEM((L, T, S // T, rows, ow), bf),
        dma((4 * L,)),
        dma((3, 4 * L, S)),
        dma((4 * L, S)),
        dma((L, T)),
        dma((L, T)),
        dma((L, S)),
        dma((L, T, S // T)),
        pltpu.VMEM((L, S, rows, ow), bf),
        dma((L, S)),
        dma((L, S)),
        dma((L, 2)),
        dma((L, 2)),
        dma((2,)),
        dma((2,)),
        dma,
    ]
    return pl.pallas_call(
        functools.partial(fused_kernel, S, T, L),
        out_shape=jax.ShapeDtypeStruct((rows, width), bf),
        in_specs=[hbm, vmem, vmem, hbm, hbm, hbm, vmem, hbm],
        out_specs=vmem,
        scratch_shapes=scratch,
        compiler_params=pltpu.CompilerParams(
            collective_id=0, has_side_effects=True, vmem_limit_bytes=60 * 1024 * 1024),
    )(stream, docs, norm_gain, gate_proj, input_gate, value_proj, jnp.transpose(taps, (1, 0, 2)), out_proj)


def solution(mesh):
    sp, tp = mesh.shape["sp"], mesh.shape["tp"]

    def body(*arrays):
        out_width = arrays[7].shape[2]
        if out_width % 128 == 0 and sp % 2 == 0 and tp % 2 == 0 and sp % tp == 0:
            return fused(sp, tp, *arrays)
        return per_device(*arrays)

    in_specs = (
        P("sp", "tp"),
        P("sp"),
        P(),
        P(None, "sp", "tp"),
        P(None, "sp", "tp"),
        P(None, "sp", "tp"),
        P(None, None, "tp"),
        P(None, "tp", "sp"),
    )
    out_specs = P("sp", "tp")
    return jax.shard_map(
        body, mesh=mesh, in_specs=in_specs, out_specs=out_specs, check_vma=False
    )
```
